32 devices in a mesh: ep: 16 (over z, y, x), tp: 2 (over core).
Axes of the slice: x: 2, y: 2, z: 4, core: 2. Of those that a mesh axis runs over, the one named last changes fastest.
Arguments:
- tokens: bfloat16 [2048, 2048], P('ep'), may hold values from -6 to 6
- cotangent: bfloat16 [2048, 2048], P('ep'), may hold values from -0.625 to 0.625
- routes: int32 [2048, 2], P('ep'), may hold values from 0 to 15, as said below
- router_group: bfloat16 [2048, 4], replicated, may hold values from -0.125 to 0.125
- router_expert: bfloat16 [2048, 16], replicated, may hold values from -0.125 to 0.125
- gate_proj: bfloat16 [16, 2048, 512], P('ep', None, 'tp'), may hold values from -0.125 to 0.125
- up_proj: bfloat16 [16, 2048, 512], P('ep', None, 'tp'), may hold values from -0.125 to 0.125
- down_proj: bfloat16 [16, 512, 2048], P('ep', 'tp'), may hold values from -0.25 to 0.25
Outputs:
- token_grad: bfloat16 [2048, 2048], P('ep', 'tp')
- gate_grad: bfloat16 [16, 2048, 512], P('ep', None, 'tp')
- up_grad: bfloat16 [16, 2048, 512], P('ep', None, 'tp')
- down_grad: bfloat16 [16, 512, 2048], P('ep', 'tp')
- gate_rows: float32 [16, 2048], P('ep')
- up_rows: float32 [16, 2048], P('ep')
- down_rows: float32 [16, 512], P('ep', 'tp')
- router_expert_grad: float32 [2048, 16], P(('ep', 'tp'))
- router_group_grad: float32 [2048, 4], P(('ep', 'tp'))
- router_rows: float32 [2048], P(('ep', 'tp'))
The draws below stay inside these ranges and needn't reach their ends.
Inputs may be any that keep to these rules, and one draw needn't show every extreme that they name: `routes`: the 2 entries of a row are different experts of one group: their quotients by 4 are equal. Among the rows of one device no expert is named more than 32 times, and the experts of one group, the same for all devices, are each named exactly 32 times by the rows of every device.
All inputs are finite; a program needn't handle non-finite values.
Results may differ from the reference program's by a relative error of at most 0.014.
Values may be sent and summed in bfloat16 or wider, within the bound.
No kernel may reach another device: no remote copies, remote signals or barrier semaphores. Data moves between devices by JAX's collectives and lax.ppermute only.
A program may use at most 64 MiB of HBM per device.

```python
import jax
import jax.numpy as jnp
from jax import lax

D = 2048
FF = 512
TOK_DEV = 128
GROUPS = 4
TOP = 2
EXPERTS = 16
GROUP_SIZE = 4
TOKENS = 2048
N_TP = 2


def draw_routes(key, part):
    blocks = TOKENS // TOK_DEV
    half_rows = TOK_DEV // 2
    others_rows = TOK_DEV - half_rows
    favored = jax.random.randint(jax.random.fold_in(key, 11), (), 0, GROUPS)
    group_ids = jnp.arange(GROUPS, dtype=jnp.int32)
    is_favored = group_ids[None, :] == favored
    shares = jax.random.randint(jax.random.fold_in(key, 12), (blocks, GROUPS), 2, 5)
    shares = jnp.where(is_favored, 0, shares)
    base_rows = others_rows * shares // jnp.sum(shares, axis=1, keepdims=True)
    leftover = others_rows - jnp.sum(base_rows, axis=1, keepdims=True)
    other_rank = jnp.cumsum(jnp.where(is_favored, 0, 1), axis=1) - 1
    extra_rows = jnp.where(jnp.logical_and(jnp.logical_not(is_favored), other_rank < leftover), 1, 0)
    counts = base_rows + extra_rows + jnp.where(is_favored, half_rows, 0)
    group_end = jnp.cumsum(counts, axis=1)
    group_start = group_end - counts
    position = jnp.arange(TOK_DEV, dtype=jnp.int32)
    labels = jnp.sum((group_end[:, None, :] <= position[None, :, None]).astype(jnp.int32), axis=2)
    within = position[None, :] - jnp.take_along_axis(group_start, labels, axis=1)
    rotate = jax.random.randint(jax.random.fold_in(key, 13), (blocks, GROUPS), 0, GROUP_SIZE)
    offset = jax.random.randint(jax.random.fold_in(key, 14), (blocks, GROUPS), 0, GROUP_SIZE - 1)
    first_pick = (within + jnp.take_along_axis(rotate, labels, axis=1)) % GROUP_SIZE
    turned = (jnp.take_along_axis(offset, labels, axis=1) + within // GROUP_SIZE) % (GROUP_SIZE - 1)
    second_pick = (first_pick + 1 + turned) % GROUP_SIZE
    chosen = jnp.stack([labels * GROUP_SIZE + first_pick, labels * GROUP_SIZE + second_pick], axis=2)
    block_keys = jax.random.split(jax.random.fold_in(key, 15), blocks)
    shuffles = jax.vmap(lambda subkey: jax.random.permutation(subkey, TOK_DEV))(block_keys)
    chosen = jnp.take_along_axis(chosen, shuffles[:, :, None], axis=1)
    return chosen.reshape(TOKENS, TOP).astype(jnp.int32)


def spiked(values, rng, source, target, blocks, factor):
    def block_of(axis_at):
        return (jnp.arange(values.shape[axis_at]) // (values.shape[axis_at] // blocks)).reshape((-1,) + (1,) * (values.ndim - 1 - axis_at))

    first = jax.random.permutation(rng, blocks)[block_of(target)]
    other_side = (block_of(target) + blocks // 2) % blocks
    return jnp.where((block_of(source) == first) | (block_of(source) == other_side), factor * values, values)


def level_of(key, shape, cuts, low, high):
    def one(dim, shards_of):
        heights = jax.random.uniform(jax.random.fold_in(jax.random.fold_in(key, 6), dim), (shards_of,), jnp.float32, low / len(cuts), high / len(cuts))
        return jnp.repeat(jnp.exp(heights), shape[dim] // shards_of).reshape((-1,) + (1,) * (len(shape) - dim - 1))

    factor_of = one(*cuts[0])
    for cut in cuts[1:]:
        factor_of = factor_of * one(*cut)
    return factor_of


def noise(key, shape, width, most, pieces=(), kind=jnp.bfloat16):
    loudness = level_of(key, shape, pieces, -0.22, 0.18) if pieces else 1.0
    result = jax.random.normal(key, shape, jnp.float32) * width * loudness
    return jnp.minimum(jnp.maximum(result, -most), most).astype(kind)


def heavy_noise(rng, extent, width, reach, pieces, heavy, kind=jnp.bfloat16):
    array = width * jax.random.normal(rng, extent, jnp.float32)
    if pieces:
        array = array * level_of(rng, extent, pieces, -0.22, 0.18)
    return jnp.clip(spiked(array, jax.random.fold_in(rng, 3), *heavy), -reach, reach).astype(kind)


def setup_inputs(seed: int = 0) -> dict:
    keys = jax.random.split(jax.random.key(seed), 9)
    tokens = heavy_noise(keys[0], (TOKENS, D), 1.0, 6.0, ((0, 16),), (0, 1, 16, 2.0))
    cotangent = noise(keys[1], (TOKENS, D), 0.1, 0.625, ((0, 16),))
    routes = draw_routes(jax.random.fold_in(keys[8], 71), 0)
    router_group = noise(keys[3], (D, GROUPS), D ** -0.5, 0.125)
    router_expert = noise(keys[4], (D, EXPERTS), D ** -0.5, 0.125)
    gate_proj = noise(keys[5], (EXPERTS, D, FF), D ** -0.5, 0.125, ((0, 16), (2, 2)))
    up_proj = noise(keys[6], (EXPERTS, D, FF), D ** -0.5, 0.125, ((0, 16), (2, 2)))
    down_proj = noise(keys[7], (EXPERTS, FF, D), FF ** -0.5, 0.25, ((0, 16), (1, 2)))
    return dict(tokens=tokens, cotangent=cotangent, routes=routes, router_group=router_group, router_expert=router_expert, gate_proj=gate_proj, up_proj=up_proj, down_proj=down_proj)


tile_rows = 128


def contract_rows(left_side, right_side):
    return lax.dot_general(left_side, right_side, (((0,), (0,)), ((), ())), preferred_element_type=jnp.float32)


def contract_cols(left_side, right_side):
    return lax.dot_general(left_side, right_side, (((1,), (1,)), ((), ())), preferred_element_type=jnp.float32)


def router_forward(tokens, routes, router_group, router_expert):
    groups = router_group.shape[1]
    experts = router_expert.shape[1]
    group_logits = jnp.dot(tokens, router_group, preferred_element_type=jnp.float32)
    expert_logits = jnp.dot(tokens, router_expert, preferred_element_type=jnp.float32)
    group_exp = jnp.exp(group_logits)
    group_prob = group_exp / jnp.sum(group_exp, axis=1, keepdims=True)
    chosen_group = routes[:, 0] // (experts // groups)
    group_onehot = (chosen_group[:, None] == jnp.arange(groups, dtype=jnp.int32)[None, :]).astype(jnp.float32)
    picked = jnp.sum(group_prob * group_onehot, axis=1)
    chosen_logits = jnp.take_along_axis(expert_logits, routes, axis=1)
    paired_exp = jnp.exp(chosen_logits)
    paired = paired_exp / jnp.sum(paired_exp, axis=1, keepdims=True)
    return group_prob, group_onehot, picked, paired


def router_backward(dweight, routes, group_prob, group_onehot, picked, paired, experts):
    dpicked = jnp.sum(dweight * paired, axis=1)
    dpaired = dweight * picked[:, None]
    dchosen = paired * (dpaired - jnp.sum(paired * dpaired, axis=1, keepdims=True))
    dgroup = ((dpicked * picked)[:, None] * (group_onehot - group_prob)).astype(jnp.bfloat16)
    expert_onehot = (routes[:, :, None] == jnp.arange(experts, dtype=jnp.int32)[None, None, :]).astype(jnp.float32)
    dexpert = jnp.sum(dchosen[:, :, None] * expert_onehot, axis=1).astype(jnp.bfloat16)
    return dgroup, dexpert


def reference(tokens, cotangent, routes, router_group, router_expert, gate_proj, up_proj, down_proj):
    group_prob, group_onehot, picked, paired = router_forward(tokens, routes, router_group, router_expert)
    weights = (picked[:, None] * paired).astype(jnp.bfloat16)
    assigned = TOKENS * TOP
    flat_ids = routes.reshape(assigned).astype(jnp.int32)
    counts = jnp.zeros((EXPERTS,), jnp.int32).at[flat_ids].add(1)
    tile_count = ((counts + (tile_rows - 1)) // tile_rows).astype(jnp.int32)
    tile_end = jnp.cumsum(tile_count).astype(jnp.int32)
    tile_begin = (tile_end - tile_count).astype(jnp.int32)
    count_begin = (jnp.cumsum(counts).astype(jnp.int32) - counts).astype(jnp.int32)
    ordering = jnp.argsort(flat_ids, stable=True).astype(jnp.int32)
    sorted_ids = flat_ids[ordering]
    ranking = jnp.arange(assigned, dtype=jnp.int32) - count_begin[sorted_ids]
    padded_pos = (tile_begin[sorted_ids] * tile_rows + ranking).astype(jnp.int32)
    tile_total = (assigned + tile_rows - 1) // tile_rows + EXPERTS
    owners = jnp.full((tile_total * tile_rows,), assigned, jnp.int32).at[padded_pos].set(ordering)
    tile_marks = jnp.arange(tile_total, dtype=jnp.int32)[:, None]
    tile_expert = jnp.minimum(jnp.sum((tile_end[None, :] <= tile_marks).astype(jnp.int32), axis=1), EXPERTS - 1).astype(jnp.int32)
    flat_weights = weights.reshape(assigned)
    piece_width = FF // N_TP

    def tile_step(totals, tile_index):
        grad_gate, grad_up, grad_down = totals
        expert = tile_expert[tile_index]
        members = lax.dynamic_slice_in_dim(owners, tile_index * tile_rows, tile_rows)
        source_rows = members // TOP
        inputs = jnp.take(tokens, source_rows, axis=0, mode="fill", fill_value=0)
        upstream = jnp.take(cotangent, source_rows, axis=0, mode="fill", fill_value=0)
        slot_scale = jnp.take(flat_weights, members, axis=0, mode="fill", fill_value=0).astype(jnp.float32)
        gate_mat = gate_proj[expert]
        up_mat = up_proj[expert]
        down_mat = down_proj[expert]
        gate_pre = jnp.dot(inputs, gate_mat, preferred_element_type=jnp.float32)
        up_pre = jnp.dot(inputs, up_mat, preferred_element_type=jnp.float32)
        sigmoid_gate = jax.nn.sigmoid(gate_pre)
        hidden = (gate_pre * sigmoid_gate * up_pre).astype(jnp.bfloat16)
        pulled = contract_cols(upstream, down_mat)
        weight_part = jnp.sum(pulled * hidden.astype(jnp.float32), axis=1)
        dhidden = slot_scale[:, None] * pulled
        gate_delta = (dhidden * up_pre * sigmoid_gate * (1.0 + gate_pre * (1.0 - sigmoid_gate))).astype(jnp.bfloat16)
        up_delta = (dhidden * gate_pre * sigmoid_gate).astype(jnp.bfloat16)
        scaled_cot = (slot_scale[:, None] * upstream.astype(jnp.float32)).astype(jnp.bfloat16)
        grad_gate = grad_gate.at[expert].add(contract_rows(inputs, gate_delta))
        grad_up = grad_up.at[expert].add(contract_rows(inputs, up_delta))
        grad_down = grad_down.at[expert].add(contract_rows(hidden, scaled_cot))
        token_total = jnp.zeros((tile_rows, D), jnp.float32)
        for piece_index in range(N_TP):
            first_col = piece_index * piece_width
            last_col = first_col + piece_width
            piece_term = contract_cols(gate_delta[:, first_col:last_col], gate_mat[:, first_col:last_col])
            piece_term = piece_term + contract_cols(up_delta[:, first_col:last_col], up_mat[:, first_col:last_col])
            token_total = token_total + piece_term.astype(jnp.bfloat16).astype(jnp.float32)
        return (grad_gate, grad_up, grad_down), (token_total.astype(jnp.bfloat16), weight_part)

    start_totals = (jnp.zeros((EXPERTS, D, FF), jnp.float32), jnp.zeros((EXPERTS, D, FF), jnp.float32),
                    jnp.zeros((EXPERTS, FF, D), jnp.float32))
    totals, tile_outputs = lax.scan(tile_step, start_totals, jnp.arange(tile_total, dtype=jnp.int32))
    grad_gate, grad_up, grad_down = totals
    token_tiles, weight_tiles = tile_outputs
    position = jnp.zeros((assigned,), jnp.int32).at[ordering].set(padded_pos)
    token_rows = token_tiles.reshape(tile_total * tile_rows, D)[position]
    expert_part = jnp.sum(token_rows.reshape(TOKENS, TOP, D).astype(jnp.float32), axis=1)
    dweight = weight_tiles.reshape(tile_total * tile_rows)[position].astype(jnp.bfloat16).astype(jnp.float32)
    dweight = dweight.reshape(TOKENS, TOP)
    dgroup, dexpert = router_backward(dweight, routes, group_prob, group_onehot, picked, paired, EXPERTS)
    router_part = contract_cols(dgroup, router_group) + contract_cols(dexpert, router_expert)
    token_grad = (expert_part + router_part).astype(jnp.bfloat16)
    router_expert_grad = contract_rows(tokens, dexpert)
    router_group_grad = contract_rows(tokens, dgroup)
    router_rows = jnp.sum(router_expert_grad * router_expert_grad, axis=1) + jnp.sum(router_group_grad * router_group_grad, axis=1)
    gate_rows = jnp.sum(grad_gate * grad_gate, axis=2)
    up_rows = jnp.sum(grad_up * grad_up, axis=2)
    down_rows = jnp.sum(grad_down * grad_down, axis=2)
    return (token_grad, grad_gate.astype(jnp.bfloat16), grad_up.astype(jnp.bfloat16), grad_down.astype(jnp.bfloat16),
            gate_rows, up_rows, down_rows, router_expert_grad, router_group_grad, router_rows)
```

```python
import functools

import jax
import jax.numpy as jnp
from jax import lax
from jax.experimental import pallas as pl
from jax.experimental.pallas import tpu as pltpu
from jax.sharding import PartitionSpec as P


BF = jnp.bfloat16
F32 = jnp.float32


def dot(a, b):
    return jnp.dot(a, b, preferred_element_type=F32)


def dot_nt(a, b):
    return lax.dot_general(a, b, (((1,), (1,)), ((), ())), preferred_element_type=F32)


def dot_tn(a, b):
    return lax.dot_general(a, b, (((0,), (0,)), ((), ())), preferred_element_type=F32)


def iota(shape, axis):
    return lax.broadcasted_iota(jnp.int32, shape, axis)


def onehot(mask):
    return jnp.where(mask, 1.0, 0.0).astype(BF)


def call(kernel, out_shapes, args, scratch=(), flops=0, in_hbm=(), limit=24 * 2**20):
    vmem = pl.BlockSpec(memory_space=pltpu.VMEM)
    smem = pl.BlockSpec(memory_space=pltpu.SMEM)
    hbm = pl.BlockSpec(memory_space=pltpu.HBM)
    in_specs = [
        smem if a.ndim == 1 and a.dtype == jnp.int32 else hbm if i in in_hbm else vmem
        for i, a in enumerate(args)
    ]
    return pl.pallas_call(
        kernel,
        out_shape=out_shapes,
        in_specs=in_specs,
        out_specs=jax.tree.map(lambda _: vmem, out_shapes),
        scratch_shapes=list(scratch),
        cost_estimate=pl.CostEstimate(flops=flops, bytes_accessed=0, transcendentals=0),
        compiler_params=pltpu.CompilerParams(vmem_limit_bytes=limit),
    )(*args)


def group_onehots(rank_row, group_row, my_group, groups, slots):
    toks = rank_row.shape[1]
    row = iota((slots, toks), 0).astype(F32)
    hit = row == rank_row
    outs = []
    for k in range(groups):
        other = jnp.bitwise_xor(my_group, k).astype(F32)
        outs.append(onehot(jnp.logical_and(hit, group_row == other)))
    return outs


def slot_hits(shape, member, cap, per, s0, s1, slot_axis):
    slot = iota(shape, slot_axis)
    block = slot // per
    want = (jnp.bitwise_xor(member, block) * cap + slot % cap + 1).astype(F32)
    return s0 == want, s1 == want


def prep_kernel(dims, ids, tok_hbm, cot_hbm, routes_hbm, rg_hbm, re_hbm, *rest):
    groups, width, cap, slots, half = dims
    outs, (tok_ref, cot_ref, routes_ref, rg_ref, re_ref, sems) = rest[:-6], rest[-6:]
    z_tok, z_cot = outs[:groups], outs[groups : 2 * groups - 1]
    own, stat_ref = outs[2 * groups - 1 : -1], outs[-1]
    toks, _ = tok_ref.shape
    experts = re_ref.shape[0]
    my_group, my_member = ids[0], ids[1]
    start = pl.multiple_of(ids[2], 128)
    copies = [
        pltpu.make_async_copy(src, dst, sems.at[i])
        for i, (src, dst) in enumerate(
            (
                (routes_hbm, routes_ref),
                (re_hbm, re_ref),
                (rg_hbm, rg_ref),
                (tok_hbm, tok_ref),
                (cot_hbm.at[:, pl.ds(start, half)], cot_ref),
            )
        )
    ]
    for copy in copies:
        copy.start()
    earlier = onehot(iota((toks, toks), 0) < iota((toks, toks), 1))
    for copy in copies[:4]:
        copy.wait()
    tokens = tok_ref[...]
    e_t = dot_nt(re_ref[...], tokens)
    g_t = dot_nt(rg_ref[...], tokens)
    g_t = jnp.concatenate([g_t, jnp.zeros((8 - groups, toks), F32)], axis=0)
    routes = routes_ref[...].astype(F32)
    r0, r1 = routes[0:1], routes[1:2]
    grow = iota((8, toks), 0)
    gexp = jnp.where(grow < groups, jnp.exp(g_t), 0.0)
    gprob = gexp / jnp.sum(gexp, axis=0, keepdims=True)
    low = (grow * width).astype(F32)
    gmask = jnp.logical_and(r0 >= low, r0 < low + width)
    picked = jnp.sum(jnp.where(gmask, gprob, 0.0), axis=0, keepdims=True)
    group_row = jnp.sum(jnp.where(gmask, grow.astype(F32), 0.0), axis=0, keepdims=True)
    erow = iota((experts, toks), 0).astype(F32)
    a0, a1 = erow == r0, erow == r1
    eexp = jnp.exp(e_t)
    x0 = jnp.sum(jnp.where(a0, eexp, 0.0), axis=0, keepdims=True)
    x1 = jnp.sum(jnp.where(a1, eexp, 0.0), axis=0, keepdims=True)
    p0, p1 = x0 / (x0 + x1), x1 / (x0 + x1)
    cum = dot(onehot(jnp.logical_or(a0, a1)), earlier)
    rank0 = jnp.sum(jnp.where(a0, cum, 0.0), axis=0, keepdims=True)
    rank1 = jnp.sum(jnp.where(a1, cum, 0.0), axis=0, keepdims=True)
    gcum = dot(onehot(gmask), earlier)
    rank_g = jnp.sum(jnp.where(gmask, gcum, 0.0), axis=0, keepdims=True)
    base = group_row * width
    s0 = (r0 - base) * cap + rank0 + 1.0
    s1 = (r1 - base) * cap + rank1 + 1.0
    mrow = iota((128, toks), 0)
    meta = jnp.where(mrow == 0, picked * p0, 0.0)
    meta = jnp.where(mrow == 1, picked * p1, meta)
    meta = jnp.where(mrow == 2, s0, meta)
    meta = jnp.where(mrow == 3, s1, meta)
    for i, v in enumerate([picked, p0, p1] + [gprob[j : j + 1] for j in range(groups)]):
        top = v.astype(BF).astype(F32)
        meta = jnp.where(mrow == 4 + 2 * i, top, meta)
        meta = jnp.where(mrow == 5 + 2 * i, v - top, meta)
    meta = meta.astype(BF)
    stat_ref[...] = jnp.where(iota((8, toks), 0) == 0, rank_g, group_row)
    sel = group_onehots(rank_g, group_row, my_group, groups, slots)
    mine = group_row == my_group.astype(F32)
    hit0, hit1 = slot_hits(
        (width * cap, toks), my_member, cap, cap,
        jnp.where(mine, s0, 0.0), jnp.where(mine, s1, 0.0), 0,
    )
    spread = onehot(jnp.logical_or(hit0, hit1))
    weight = dot_nt(onehot(hit0), meta)[:, 0:1] + dot_nt(onehot(hit1), meta)[:, 1:2]
    every = jnp.concatenate(sel + [spread], axis=0)
    metas = dot_nt(jnp.concatenate(sel, axis=0), meta).astype(BF)
    first = groups * slots
    moved_tok = dot(every, tok_ref[:, pl.ds(start, half)]).astype(BF)
    for k in range(groups):
        z_tok[k][:, :half] = moved_tok[k * slots : (k + 1) * slots]
        z_tok[k][:, half:] = metas[k * slots : (k + 1) * slots]
    copies[4].wait()
    moved_cot = dot(every[slots:], cot_ref[...]).astype(BF)
    for k in range(1, groups):
        z_cot[k - 1][...] = moved_cot[(k - 1) * slots : k * slots]
    wide = jnp.broadcast_to(weight, (width * cap, 128)).astype(BF)
    for k in range(width):
        at = first + k * cap
        own[k][:, :half] = moved_tok[at : at + cap]
        own[k][:, half : 2 * half] = moved_cot[at - slots : at - slots + cap]
        own[k][:, 2 * half :] = wide[k * cap : (k + 1) * cap]


def spread_kernel(dims, with_weight, ids, *refs):
    groups, width, cap, slots, half = dims
    srcs = groups - 1
    z, outs = refs[: len(refs) - width], refs[len(refs) - width :]
    tok = z[:srcs]
    meta = jnp.concatenate([r[:, half:] for r in tok], axis=0).astype(F32)
    rows = jnp.transpose(meta)
    data = tok if with_weight else z[srcs:]
    data = jnp.concatenate([r[:, :half] for r in data], axis=0)
    shape = (width * srcs * cap, srcs * slots)
    same = iota(shape, 0) // cap % srcs == iota(shape, 1) // slots
    hit0, hit1 = slot_hits(shape, ids[1], cap, srcs * cap, rows[2:3], rows[3:4], 0)
    hit0, hit1 = jnp.logical_and(same, hit0), jnp.logical_and(same, hit1)
    spread = dot(onehot(jnp.logical_or(hit0, hit1)), data).astype(BF)
    per = srcs * cap
    if with_weight:
        meta = meta.astype(BF)
        weight = dot(onehot(hit0), meta)[:, 0:1] + dot(onehot(hit1), meta)[:, 1:2]
        wide = jnp.broadcast_to(weight, (width * per, 128)).astype(BF)
    for k in range(width):
        outs[k][:, :half] = spread[k * per : (k + 1) * per]
        if with_weight:
            outs[k][:, half:] = wide[k * per : (k + 1) * per]


def assemble(ids, own, other, out_ref, half, at):
    mine = pl.multiple_of(ids[2], 128)
    theirs = pl.multiple_of(half - ids[2], 128)
    width = len(own[0])
    rows = out_ref.shape[0] // width
    for base, (first, second) in ((mine, own), (theirs, other)):
        for k in range(width):
            low = first[k].shape[0]
            out_ref[k * rows : k * rows + low, pl.ds(base, half)] = first[k][:, at : at + half]
            out_ref[k * rows + low : (k + 1) * rows, pl.ds(base, half)] = second[k][:, :half]


def forward_kernel(width, half, ids, *refs):
    parts = [refs[i * width : (i + 1) * width] for i in range(4)]
    gate_ref, up_ref, x_ref, gp_ref, upp_ref = refs[4 * width :]
    assemble(ids, parts[:2], parts[2:], x_ref, half, 0)
    x = x_ref[...]
    gp_ref[...] = dot(x, gate_ref[...])
    upp_ref[...] = dot(x, up_ref[...])


def delta_kernel(width, half, ids, *refs):
    parts = [refs[i * width : (i + 1) * width] for i in range(4)]
    tok = refs[4 * width : 5 * width]
    down_ref, gp_ref, upp_ref, gd_ref, ud_ref, hid_ref, c_ref, w_ref, s_ref = refs[5 * width :]
    assemble(ids, parts[:2], parts[2:], c_ref, half, half)
    rows = c_ref.shape[0] // width
    for k in range(width):
        low = parts[0][k].shape[0]
        w_ref[k * rows : k * rows + low, :] = parts[0][k][:, 2 * half :].astype(F32)
        w_ref[k * rows + low : (k + 1) * rows, :] = tok[k][:, half:].astype(F32)
    pulled = dot_nt(c_ref[...], down_ref[...])
    gate_pre, up_pre = gp_ref[...], upp_ref[...]
    sig = 1.0 / (1.0 + jnp.exp(-gate_pre))
    silu = gate_pre * sig
    hidden = (silu * up_pre).astype(BF)
    hid_ref[...] = hidden
    dh = w_ref[:, 0:1] * pulled
    gd_ref[...] = (dh * up_pre * sig * (1.0 + gate_pre * (1.0 - sig))).astype(BF)
    ud_ref[...] = (dh * silu).astype(BF)
    part = jnp.sum(pulled * hidden.astype(F32), axis=1, keepdims=True)
    top = part.astype(BF).astype(F32)
    lane = iota((part.shape[0], 128), 1)
    s_ref[...] = jnp.where(lane == 0, top, jnp.where(lane == 1, part - top, 0.0)).astype(BF)


def term_kernel(own, width, half, ids, gd_ref, ud_ref, gate_ref, up_ref, s_ref, *outs):
    base = ids[2] if own else half - ids[2]
    rows = outs[0].shape[0]
    gd, ud = gd_ref[...], ud_ref[...]
    step = 256
    for k in range(width):
        outs[k][:, half:] = s_ref[k * rows : (k + 1) * rows, :]

    @pl.loop(0, half // step)
    def _(i):
        at = pl.ds(pl.multiple_of(base + i * step, step), step)
        term = dot_nt(gd, gate_ref[at, :]) + dot_nt(ud, up_ref[at, :])
        to = pl.ds(pl.multiple_of(i * step, step), step)
        for k in range(width):
            outs[k][:, to] = term[k * rows : (k + 1) * rows].astype(BF)


def add_kernel(width, half, *refs):
    for k in range(width):
        total = refs[k][...].astype(F32) + refs[width + k][...].astype(F32)
        out = refs[2 * width + k]
        out[:, :half] = total[:, :half].astype(BF)
        tail = total[:, half : half + 1] + total[:, half + 1 : half + 2]
        out[:, half:] = jnp.broadcast_to(tail, (total.shape[0], 128)).astype(BF)


def grad_kernel(x_ref, gd_ref, ud_ref, gg_ref, ug_ref, gsq_ref, usq_ref):
    step = 256

    @pl.loop(0, x_ref.shape[1] // step)
    def _(i):
        at = pl.ds(pl.multiple_of(i * step, step), step)
        xt = jnp.transpose(x_ref[:, at])
        for d_ref, out, sq in ((gd_ref, gg_ref, gsq_ref), (ud_ref, ug_ref, usq_ref)):
            total = dot(xt, d_ref[...])
            out[at, :] = total.astype(BF)
            part = jnp.sum(total * total, axis=1, keepdims=True)
            sq[:, at] = jnp.transpose(jnp.broadcast_to(part, (step, 128)))[:1]


def down_kernel(c_ref, w_ref, hid_ref, out_ref, sq_ref, acc, hid_t):
    step = 256
    acc[...] = jnp.zeros_like(acc)
    hid_t[...] = jnp.transpose(hid_ref[...])

    @pl.loop(0, c_ref.shape[1] // step)
    def _(i):
        at = pl.ds(pl.multiple_of(i * step, step), step)
        scaled = (w_ref[:, 0:1] * c_ref[:, at].astype(F32)).astype(BF)
        total = dot(hid_t[...], scaled)
        out_ref[:, at] = total.astype(BF)
        acc[...] += jnp.sum(total * total, axis=1, keepdims=True)

    sq_ref[...] = jnp.transpose(jnp.broadcast_to(acc[...], (acc.shape[0], 128)))[:1]


def reduce_kernel(dims, got_ref, e_ref, g_ref, rows_ref):
    experts, groups, own = dims
    total = jnp.sum(got_ref[...], axis=0)
    pack = 128 // own
    total = jnp.concatenate([total[:, i * own : (i + 1) * own] for i in range(pack)], axis=0)
    by_expert, by_group = total[:experts], total[experts : experts + groups]
    e_ref[...] = by_expert
    g_ref[...] = by_group
    rows_ref[...] = jnp.sum(by_expert * by_expert, axis=0, keepdims=True) + jnp.sum(
        by_group * by_group, axis=0, keepdims=True
    )


def merge_kernel(dims, experts, ids, rt_ref, *refs):
    groups, width, cap, slots, half = dims
    blocks, tok = refs[:width], refs[width : width + groups]
    outs, (mine_ref, other_ref) = refs[width + groups : -2], refs[-2:]
    start = pl.multiple_of(ids[2], 128)
    meta = jnp.concatenate([r[:, half:] for r in tok], axis=0).astype(F32)
    shape = (groups * slots, width * groups * cap)
    same = iota(shape, 1) // cap % groups == iota(shape, 0) // slots
    hit0, hit1 = slot_hits(shape, ids[1], cap, groups * cap, meta[:, 2:3], meta[:, 3:4], 1)
    hit0, hit1 = jnp.logical_and(same, hit0), jnp.logical_and(same, hit1)
    sent = jnp.concatenate([r[:, half:] for r in blocks], axis=0)
    lane = iota(meta.shape, 1)
    meta = jnp.where(lane == 126, dot(onehot(hit0), sent), meta)
    meta = jnp.where(lane == 127, dot(onehot(hit1), sent), meta)
    rows = jnp.transpose(meta)
    picked, p0, p1 = [rows[4 + 2 * i : 5 + 2 * i] + rows[5 + 2 * i : 6 + 2 * i] for i in range(3)]
    s0, s1 = rows[126:127], rows[127:128]
    dpicked = s0 * p0 + s1 * p1
    q0, q1 = picked * s0, picked * s1
    mean = p0 * q0 + p1 * q1
    c0, c1 = p0 * (q0 - mean), p1 * (q1 - mean)
    toks = groups * slots
    grow = iota((8, toks), 0)
    dgroup = jnp.zeros((8, toks), F32)
    for j in range(groups):
        at = 10 + 2 * j
        prob = rows[at : at + 1] + rows[at + 1 : at + 2]
        hot = jnp.where(ids[0] == j, 1.0, 0.0)
        dgroup = jnp.where(grow == j, dpicked * picked * (hot - prob), dgroup)
    low = ids[0] * width
    erow = ((iota((experts, toks), 0) - low) * cap).astype(F32)
    dexpert = jnp.zeros((experts, toks), F32)
    for c, slot in ((c0, rows[2:3]), (c1, rows[3:4])):
        inside = jnp.logical_and(slot > erow, slot <= erow + cap)
        dexpert += jnp.where(inside, c, 0.0)
    d = jnp.concatenate([dexpert, dgroup], axis=0).astype(BF)
    hit = onehot(jnp.logical_or(hit0, hit1))
    total = dot(hit, jnp.concatenate([r[:, :half] for r in blocks], axis=0))
    total += dot_tn(d, rt_ref[:, pl.ds(start, half)])
    for j in range(groups):
        outs[j][...] = total[j * slots : (j + 1) * slots].astype(BF)
    part = dot(d, jnp.concatenate([r[:, :half] for r in tok], axis=0))
    count, high = mine_ref.shape[:2]
    own = half // (2 * count)
    pack = 128 // own
    part = jnp.concatenate([part, jnp.zeros((high * pack - part.shape[0], half), F32)], axis=0)
    for j in range(count):
        low, up = part[:, 2 * j * own : (2 * j + 1) * own], part[:, (2 * j + 1) * own : (2 * j + 2) * own]
        for ref, cols in (
            (mine_ref, jnp.where(ids[3] == 0, low, up)),
            (other_ref, jnp.where(ids[3] == 0, up, low)),
        ):
            ref[j] = jnp.concatenate(
                [cols[i * high : (i + 1) * high] for i in range(pack)], axis=1
            )


def final_kernel(dims, ids, stat_ref, *refs):
    groups, slots = dims
    blocks, out_ref = refs[:groups], refs[groups]
    sel = group_onehots(stat_ref[0:1, :], stat_ref[1:2, :], ids[0], groups, slots)
    every = jnp.concatenate(sel, axis=0)
    out_ref[...] = dot_tn(every, jnp.concatenate([r[...] for r in blocks], axis=0)).astype(BF)


def body(tokens, cotangent, routes, router_group, router_expert, gate_proj, up_proj, down_proj):
    toks, model = tokens.shape
    top = routes.shape[1]
    groups = router_group.shape[1]
    experts = router_expert.shape[1]
    width = experts // groups
    cap = toks // width
    slots = width * cap // top
    ep = lax.axis_size("ep")
    tp = lax.axis_size("tp")
    half = model // tp
    hidden = gate_proj.shape[2]
    rows = groups * cap
    total_rows = width * rows
    ep_i, tp_i = lax.axis_index("ep"), lax.axis_index("tp")
    ids = jnp.stack([ep_i // width, ep_i % width, tp_i * half, tp_i]).astype(jnp.int32)
    dims = (groups, width, cap, slots, half)

    def sds(shape, dtype=BF):
        return jax.ShapeDtypeStruct(shape, dtype)

    def over_groups(blocks):
        moved = []
        for k, x in enumerate(blocks, 1):
            perm = [(i, ((i // width) ^ k) * width + i % width) for i in range(ep)]
            moved.append(lax.ppermute(x, "ep", perm))
        return moved

    def over_members(blocks):
        moved = [blocks[0]]
        for k in range(1, width):
            moved.append(lax.ppermute(blocks[k], "ep", [(i, i ^ k) for i in range(ep)]))
        return moved

    def swap(x):
        return lax.ppermute(x, "tp", [(i, tp - 1 - i) for i in range(tp)])

    def swaps(blocks):
        return [swap(x) for x in blocks]

    flat = total_rows * model * hidden
    small = toks * toks * model
    srcs = groups - 1
    prep = call(
        functools.partial(prep_kernel, dims),
        [sds((slots, half + 128))] * groups
        + [sds((slots, half))] * srcs
        + [sds((cap, model + 128))] * width
        + [sds((8, toks), F32)],
        (ids, tokens, cotangent, routes.T, router_group.T, router_expert.T),
        scratch=[
            pltpu.VMEM((toks, model), BF),
            pltpu.VMEM((toks, half), BF),
            pltpu.VMEM((top, toks), jnp.int32),
            pltpu.VMEM((groups, model), BF),
            pltpu.VMEM((experts, model), BF),
            pltpu.SemaphoreType.DMA((5,)),
        ],
        in_hbm=(1, 2, 3, 4, 5),
        limit=60 * 2**20,
        flops=4 * small,
    )
    z_tok, z_cot, near, stat = (
        prep[:groups], prep[groups : groups + srcs], prep[groups + srcs : -1], prep[-1],
    )
    z_own, z_tok = z_tok[0], over_groups(z_tok[1:])
    z_cot = over_groups(z_cot)
    near = over_members(near)
    m_tok = call(
        functools.partial(spread_kernel, dims, True),
        [sds((srcs * cap, half + 128))] * width,
        (ids, *z_tok),
        flops=4 * small,
    )
    m_tok = over_members(m_tok)
    m_cot = call(
        functools.partial(spread_kernel, dims, False),
        [sds((srcs * cap, half))] * width,
        (ids, *z_tok, *z_cot),
        flops=4 * small,
    )
    m_cot = over_members(m_cot)
    o_near = swaps(near)
    o_tok = swaps(m_tok)
    o_cot = swaps(m_cot)
    gate_mat, up_mat, down_mat = gate_proj[0], up_proj[0], down_proj[0]
    x_full, gate_pre, up_pre = call(
        functools.partial(forward_kernel, width, half),
        [
            sds((total_rows, model)),
            sds((total_rows, hidden), F32),
            sds((total_rows, hidden), F32),
        ],
        (ids, *near, *m_tok, *o_near, *o_tok, gate_mat, up_mat),
        flops=4 * flat,
    )
    gate_delta, up_delta, hid, c_full, w_cols, s_part = call(
        functools.partial(delta_kernel, width, half),
        [sds((total_rows, hidden))] * 3
        + [sds((total_rows, model)), sds((total_rows, 128), F32), sds((total_rows, 128))],
        (ids, *near, *m_cot, *o_near, *o_cot, *m_tok, down_mat, gate_pre, up_pre),
        flops=2 * flat,
    )
    terms = []
    for own in (False, True):
        terms.append(
            call(
                functools.partial(term_kernel, own, width, half),
                [sds((rows, half + 128))] * width,
                (ids, gate_delta, up_delta, gate_mat, up_mat, s_part),
                flops=2 * flat,
            )
        )
    back = call(
        functools.partial(add_kernel, width, half),
        [sds((rows, half + 128))] * width,
        (*terms[1], *swaps(terms[0])),
        flops=small,
    )
    back = over_members(back)
    gate_grad, up_grad, gsq, usq = call(
        grad_kernel,
        [sds((model, hidden))] * 2 + [sds((1, model), F32)] * 2,
        (x_full, gate_delta, up_delta),
        flops=4 * flat,
    )
    down_grad, dsq = call(
        down_kernel,
        [sds((hidden, model)), sds((1, hidden), F32)],
        (c_full, w_cols, hid),
        scratch=[pltpu.VMEM((hidden, 1), F32), pltpu.VMEM((hidden, total_rows), BF)],
        flops=2 * flat,
    )
    own = model // (ep * tp)
    high = -(-(experts + 8) // (8 * (128 // own))) * 8
    routers = jnp.concatenate(
        [router_expert.T, router_group.T, jnp.zeros((8 - groups, model), BF)], axis=0
    )
    merged = call(
        functools.partial(merge_kernel, dims, experts),
        [sds((slots, half))] * groups + [sds((ep // tp, high, 128), F32)] * 2,
        (ids, routers, *back, z_own, *z_tok),
        flops=4 * small,
    )
    b_z, mine, other = merged[:groups], merged[-2], merged[-1]
    b_z = [b_z[0]] + over_groups(b_z[1:])
    other = swap(other)
    part = jnp.where(
        tp_i == 0,
        jnp.concatenate([mine, other], axis=0),
        jnp.concatenate([other, mine], axis=0),
    )
    part = lax.all_to_all(part, "ep", split_axis=0, concat_axis=0, tiled=True)
    by_expert, by_group, router_rows = call(
        functools.partial(reduce_kernel, (experts, groups, own)),
        [sds((experts, own), F32), sds((groups, own), F32), sds((1, own), F32)],
        (part,),
        flops=small // 8,
    )
    token_grad = call(
        functools.partial(final_kernel, (groups, slots)),
        sds((toks, half)),
        (ids, stat, *b_z),
        flops=2 * small,
    )
    gsq = gsq + swap(gsq)
    usq = usq + swap(usq)
    return (
        token_grad,
        gate_grad[None],
        up_grad[None],
        down_grad[None],
        gsq,
        usq,
        dsq,
        by_expert.T,
        by_group.T,
        router_rows.reshape(own),
    )


def solution(mesh):
    return jax.shard_map(
        body,
        mesh=mesh,
        in_specs=(
            P("ep", None),
            P("ep", None),
            P("ep", None),
            P(),
            P(),
            P("ep", None, "tp"),
            P("ep", None, "tp"),
            P("ep", "tp", None),
        ),
        out_specs=(
            P("ep", "tp"),
            P("ep", None, "tp"),
            P("ep", None, "tp"),
            P("ep", "tp", None),
            P("ep", None),
            P("ep", None),
            P("ep", "tp"),
            P(("ep", "tp"), None),
            P(("ep", "tp"), None),
            P(("ep", "tp")),
        ),
        check_vma=False,
    )
```

```python
import functools

import jax
import jax.numpy as jnp
from jax import lax
from jax.experimental import pallas as pl
from jax.experimental.pallas import tpu as pltpu
from jax.sharding import PartitionSpec as P


BF = jnp.bfloat16
F32 = jnp.float32


def dot(a, b):
    return jnp.dot(a, b, preferred_element_type=F32)


def dot_nt(a, b):
    return lax.dot_general(a, b, (((1,), (1,)), ((), ())), preferred_element_type=F32)


def dot_tn(a, b):
    return lax.dot_general(a, b, (((0,), (0,)), ((), ())), preferred_element_type=F32)


def iota(shape, axis):
    return lax.broadcasted_iota(jnp.int32, shape, axis)


def onehot(mask):
    return jnp.where(mask, 1.0, 0.0).astype(BF)


def where_am_i(width):
    ep, tp = lax.axis_index("ep"), lax.axis_index("tp")
    return ep // width, ep % width, tp


def call(kernel, out_shapes, args, scratch=(), flops=0, in_hbm=(), limit=24 * 2**20):
    vmem = pl.BlockSpec(memory_space=pltpu.VMEM)
    smem = pl.BlockSpec(memory_space=pltpu.SMEM)
    hbm = pl.BlockSpec(memory_space=pltpu.HBM)
    in_specs = [
        smem if a.ndim == 1 and a.dtype == jnp.int32 else hbm if i in in_hbm else vmem
        for i, a in enumerate(args)
    ]
    return pl.pallas_call(
        kernel,
        out_shape=out_shapes,
        in_specs=in_specs,
        out_specs=jax.tree.map(lambda _: vmem, out_shapes),
        scratch_shapes=list(scratch),
        cost_estimate=pl.CostEstimate(flops=flops, bytes_accessed=0, transcendentals=0),
        compiler_params=pltpu.CompilerParams(vmem_limit_bytes=limit),
    )(*args)


def group_onehots(rank_row, group_row, my_group, ks, slots):
    toks = rank_row.shape[1]
    hit = iota((slots, toks), 0).astype(F32) == rank_row
    outs = []
    for k in ks:
        other = jnp.bitwise_xor(my_group, k).astype(F32)
        outs.append(onehot(jnp.logical_and(hit, group_row == other)))
    return jnp.concatenate(outs, axis=0)


def slot_hits(shape, member, cap, per, s0, s1, slot_axis):
    slot = iota(shape, slot_axis)
    block = slot // per
    want = (jnp.bitwise_xor(member, block) * cap + slot % cap + 1).astype(F32)
    return s0 == want, s1 == want


def prep_kernel(dims, tok_hbm, cot_hbm, routes_hbm, rg_hbm, re_hbm, *rest):
    groups, width, cap, slots = dims
    near_ref, tok_out, cot_out, stat_ref, tok_ref, cot_ref, routes_ref, rg_ref, re_ref, sems = rest
    toks, model = tok_ref.shape
    experts = re_ref.shape[0]
    my_group, _, core = where_am_i(width)
    copies = [
        pltpu.make_async_copy(src, dst, sems.at[i])
        for i, (src, dst) in enumerate(
            (
                (routes_hbm, routes_ref),
                (re_hbm, re_ref),
                (rg_hbm, rg_ref),
                (tok_hbm, tok_ref),
                (cot_hbm, cot_ref),
            )
        )
    ]
    for copy in copies:
        copy.start()
    earlier = onehot(iota((toks, toks), 0) < iota((toks, toks), 1))
    for copy in copies[:4]:
        copy.wait()
    tokens = tok_ref[...]
    e_t = dot_nt(re_ref[...], tokens)
    g_t = dot_nt(rg_ref[...], tokens)
    g_t = jnp.concatenate([g_t, jnp.zeros((8 - groups, toks), F32)], axis=0)
    routes = routes_ref[...].astype(F32)
    r0, r1 = routes[0:1], routes[1:2]
    grow = iota((8, toks), 0)
    gexp = jnp.where(grow < groups, jnp.exp(g_t), 0.0)
    gprob = gexp / jnp.sum(gexp, axis=0, keepdims=True)
    low = (grow * width).astype(F32)
    gmask = jnp.logical_and(r0 >= low, r0 < low + width)
    picked = jnp.sum(jnp.where(gmask, gprob, 0.0), axis=0, keepdims=True)
    group_row = jnp.sum(jnp.where(gmask, grow.astype(F32), 0.0), axis=0, keepdims=True)
    erow = iota((experts, toks), 0).astype(F32)
    a0, a1 = erow == r0, erow == r1
    eexp = jnp.exp(e_t)
    x0 = jnp.sum(jnp.where(a0, eexp, 0.0), axis=0, keepdims=True)
    x1 = jnp.sum(jnp.where(a1, eexp, 0.0), axis=0, keepdims=True)
    p0, p1 = x0 / (x0 + x1), x1 / (x0 + x1)
    cum = dot(onehot(jnp.logical_or(a0, a1)), earlier)
    rank0 = jnp.sum(jnp.where(a0, cum, 0.0), axis=0, keepdims=True)
    rank1 = jnp.sum(jnp.where(a1, cum, 0.0), axis=0, keepdims=True)
    gcum = dot(onehot(gmask), earlier)
    rank_g = jnp.sum(jnp.where(gmask, gcum, 0.0), axis=0, keepdims=True)
    base = group_row * width
    s0 = (r0 - base) * cap + rank0 + 1.0
    s1 = (r1 - base) * cap + rank1 + 1.0
    mrow = iota((128, toks), 0)
    meta = jnp.where(mrow == 0, picked * p0, 0.0)
    meta = jnp.where(mrow == 1, picked * p1, meta)
    meta = jnp.where(mrow == 2, s0, meta)
    meta = jnp.where(mrow == 3, s1, meta)
    for i, v in enumerate([picked, p0, p1] + [gprob[j : j + 1] for j in range(groups)]):
        top = v.astype(BF).astype(F32)
        meta = jnp.where(mrow == 4 + 2 * i, top, meta)
        meta = jnp.where(mrow == 5 + 2 * i, v - top, meta)
    meta = meta.astype(BF)
    stat_ref[...] = jnp.where(iota((8, toks), 0) == 0, rank_g, group_row)
    every = group_onehots(rank_g, group_row, my_group, (core, groups - 1 - core), slots)
    metas = dot_nt(every, meta).astype(BF)
    moved = dot(every, tokens).astype(BF)
    near_ref[:, :model] = moved[:slots]
    tok_out[:, :model] = moved[slots:]
    near_ref[:, 2 * model :] = metas[:slots]
    tok_out[:, model:] = metas[slots:]
    copies[4].wait()
    moved = dot(every, cot_ref[...]).astype(BF)
    near_ref[:, model : 2 * model] = moved[:slots]
    cot_out[...] = moved[slots:]


def spread_kernel(dims, meta_ref, *refs):
    _, width, cap, slots = dims
    member = where_am_i(width)[1]
    data, outs = refs[: len(refs) - width], refs[len(refs) - width :]
    tail = meta_ref.shape[1] - 128
    meta = meta_ref[:, tail:]
    rows = jnp.transpose(jnp.concatenate([meta.astype(F32), jnp.zeros((128 - slots, 128), F32)], axis=0))
    rows = rows[:, :slots]
    shape = (width * cap, slots)
    hit0, hit1 = slot_hits(shape, member, cap, cap, rows[2:3], rows[3:4], 0)
    hit0, hit1 = onehot(hit0), onehot(hit1)
    values = data[0][...] if data else meta_ref[:, :tail]
    spread = dot(hit0 + hit1, values).astype(BF)
    for k in range(width):
        outs[k][:, : values.shape[1]] = spread[k * cap : (k + 1) * cap]
    if not data:
        weight = dot(hit0, meta)[:, 0:1] + dot(hit1, meta)[:, 1:2]
        wide = jnp.broadcast_to(weight, (width * cap, 128)).astype(BF)
        for k in range(width):
            outs[k][:, tail:] = wide[k * cap : (k + 1) * cap]


def forward_kernel(width, *refs):
    first, second = refs[:width], refs[width : 2 * width]
    weights, x_ref, outs = refs[2 * width : 2 * width + 4], refs[-5], refs[-4:]
    model = x_ref.shape[1]
    cap = first[0].shape[0]
    for k in range(width):
        x_ref[k * cap : (k + 1) * cap, :] = first[k][:, :model]
        x_ref[(width + k) * cap : (width + k + 1) * cap, :] = second[k][:, :model]
    x = x_ref[...]
    for w, out in zip(weights, outs):
        out[...] = dot(x, w[...])


def delta_kernel(width, *refs):
    first, second, tok = refs[:width], refs[width : 2 * width], refs[2 * width : 3 * width]
    gates, ups, downs = refs[3 * width : 3 * width + 2], refs[3 * width + 2 : 3 * width + 4], refs[3 * width + 4 : 3 * width + 6]
    gps, upps = refs[3 * width + 6 : 3 * width + 8], refs[3 * width + 8 : 3 * width + 10]
    outs = refs[3 * width + 10 :]
    mine_ref, other_ref, c_ref, w_ref = outs[:4]
    backs = outs[4 : 4 + width]
    model = c_ref.shape[1]
    cap = first[0].shape[0]
    for k in range(width):
        low, up = slice(k * cap, (k + 1) * cap), slice((width + k) * cap, (width + k + 1) * cap)
        c_ref[low, :] = first[k][:, model : 2 * model]
        c_ref[up, :] = second[k][...]
        w_ref[low, :] = first[k][:, 2 * model :].astype(F32)
        w_ref[up, :] = tok[k][:, model:].astype(F32)
    c = c_ref[...]
    scale = w_ref[:, 0:1]
    hidden = gates[0].shape[1]
    s = None
    for n, out in enumerate((mine_ref, other_ref)):
        pulled = dot_nt(c, downs[n][...])
        gate_pre, up_pre = gps[n][...], upps[n][...]
        sig = 1.0 / (1.0 + jnp.exp(-gate_pre))
        silu = gate_pre * sig
        hid = (silu * up_pre).astype(BF)
        dh = scale * pulled
        out[:, :hidden] = (dh * up_pre * sig * (1.0 + gate_pre * (1.0 - sig))).astype(BF)
        out[:, hidden : 2 * hidden] = (dh * silu).astype(BF)
        out[:, 2 * hidden :] = hid
        part = jnp.sum(pulled * hid.astype(F32), axis=1, keepdims=True)
        s = part if s is None else s + part
    wide = jnp.broadcast_to(s, (s.shape[0], 128)).astype(BF)
    for k in range(width):
        backs[k][:cap, model:] = wide[k * cap : (k + 1) * cap]
        backs[k][cap:, model:] = wide[(width + k) * cap : (width + k + 1) * cap]
    step = 256

    @pl.loop(0, model // step)
    def _(i):
        at = pl.ds(pl.multiple_of(i * step, step), step)
        term = None
        for n, out in enumerate((mine_ref, other_ref)):
            piece = dot_nt(out[:, :hidden], gates[n][at, :])
            piece += dot_nt(out[:, hidden : 2 * hidden], ups[n][at, :])
            term = piece if term is None else term + piece
        term = term.astype(BF)
        for k in range(width):
            backs[k][:cap, at] = term[k * cap : (k + 1) * cap]
            backs[k][cap:, at] = term[(width + k) * cap : (width + k + 1) * cap]


def scale_kernel(c_ref, w_ref, out_ref):
    out_ref[...] = (w_ref[:, 0:1] * c_ref[...].astype(F32)).astype(BF)


def fold(x):
    total = x[:, :128]
    for i in range(1, x.shape[1] // 128):
        total = total + x[:, i * 128 : (i + 1) * 128]
    return total


def grad_kernel(x_ref, other_ref, mine_ref, got_ref, gg_ref, ug_ref, sq_ref, gd_ref, ud_ref):
    rows, hidden = x_ref.shape[0], gd_ref.shape[1]
    for n, ref in enumerate((mine_ref, got_ref)):
        gd_ref[n * rows : (n + 1) * rows, :] = ref[:, :hidden]
        ud_ref[n * rows : (n + 1) * rows, :] = ref[:, hidden : 2 * hidden]
    step = 512

    @pl.loop(0, x_ref.shape[1] // step)
    def _(i):
        at = pl.ds(pl.multiple_of(i * step, step), step)
        xt = jnp.concatenate(
            [jnp.transpose(x_ref[:, at]), jnp.transpose(other_ref[:, at])], axis=1
        )
        for n, (d_ref, out) in enumerate(((gd_ref, gg_ref), (ud_ref, ug_ref))):
            total = dot(xt, d_ref[...])
            out[at, :] = total.astype(BF)
            part = jnp.transpose(fold(total * total))
            sq_ref[n : n + 1, at] = jnp.sum(part, axis=0, keepdims=True)


def down_kernel(c_ref, other_ref, mine_ref, got_ref, out_ref, sq_ref, acc, hid_t):
    rows, hidden = c_ref.shape[0], hid_t.shape[0]
    acc[...] = jnp.zeros_like(acc)
    hid_t[:, :rows] = jnp.transpose(mine_ref[:, 2 * hidden :])
    hid_t[:, rows:] = jnp.transpose(got_ref[:, 2 * hidden :])
    step = 512

    @pl.loop(0, c_ref.shape[1] // step)
    def _(i):
        at = pl.ds(pl.multiple_of(i * step, step), step)
        total = dot(hid_t[...], jnp.concatenate([c_ref[:, at], other_ref[:, at]], axis=0))
        out_ref[:, at] = total.astype(BF)
        acc[...] += fold(total * total)

    sq_ref[...] = jnp.sum(jnp.transpose(acc[...]), axis=0, keepdims=True)


def reduce_kernel(dims, got_ref, sq_ref, sq_other_ref, e_ref, g_ref, rows_ref, gsq_ref, usq_ref):
    experts, groups, own = dims
    total = jnp.sum(got_ref[...], axis=0)
    pack = 128 // own
    total = jnp.concatenate([total[:, i * own : (i + 1) * own] for i in range(pack)], axis=0)
    by_expert, by_group = total[:experts], total[experts : experts + groups]
    e_ref[...] = by_expert
    g_ref[...] = by_group
    rows_ref[...] = jnp.sum(by_expert * by_expert, axis=0, keepdims=True) + jnp.sum(
        by_group * by_group, axis=0, keepdims=True
    )
    gsq_ref[...] = sq_ref[0:1] + sq_other_ref[0:1]
    usq_ref[...] = sq_ref[1:2] + sq_other_ref[1:2]


def merge_kernel(dims, experts, rt_ref, near_ref, tok_ref, *refs):
    groups, width, cap, slots = dims
    blocks, (y0_ref, y1_ref, mine_ref, other_ref) = refs[:width], refs[width:]
    my_group, member, core = where_am_i(width)
    model = y0_ref.shape[1]
    meta = jnp.concatenate([near_ref[:, 2 * model :], tok_ref[:, model:]], axis=0).astype(F32)
    toks = 2 * slots
    shape = (toks, width * 2 * cap)
    same = iota(shape, 1) // cap % 2 == iota(shape, 0) // slots
    hit0, hit1 = slot_hits(shape, member, cap, 2 * cap, meta[:, 2:3], meta[:, 3:4], 1)
    hit0, hit1 = onehot(jnp.logical_and(same, hit0)), onehot(jnp.logical_and(same, hit1))
    sent = jnp.concatenate([r[:, model:] for r in blocks], axis=0)
    lane = iota(meta.shape, 1)
    meta = jnp.where(lane == 126, dot(hit0, sent), meta)
    meta = jnp.where(lane == 127, dot(hit1, sent), meta)
    rows = jnp.transpose(meta)
    picked, p0, p1 = [rows[4 + 2 * i : 5 + 2 * i] + rows[5 + 2 * i : 6 + 2 * i] for i in range(3)]
    s0, s1 = rows[126:127], rows[127:128]
    dpicked = s0 * p0 + s1 * p1
    q0, q1 = picked * s0, picked * s1
    mean = p0 * q0 + p1 * q1
    c0, c1 = p0 * (q0 - mean), p1 * (q1 - mean)
    grow = iota((8, toks), 0)
    dgroup = jnp.zeros((8, toks), F32)
    for j in range(groups):
        at = 10 + 2 * j
        prob = rows[at : at + 1] + rows[at + 1 : at + 2]
        hot = jnp.where(my_group == j, 1.0, 0.0)
        dgroup = jnp.where(grow == j, dpicked * picked * (hot - prob), dgroup)
    erow = ((iota((experts, toks), 0) - my_group * width) * cap).astype(F32)
    dexpert = jnp.zeros((experts, toks), F32)
    for c, slot in ((c0, rows[2:3]), (c1, rows[3:4])):
        inside = jnp.logical_and(slot > erow, slot <= erow + cap)
        dexpert += jnp.where(inside, c, 0.0)
    d = jnp.concatenate([dexpert, dgroup], axis=0).astype(BF)
    total = dot(hit0 + hit1, jnp.concatenate([r[:, :model] for r in blocks], axis=0))
    total += dot_tn(d, rt_ref[...])
    y0_ref[...] = total[:slots].astype(BF)
    y1_ref[...] = total[slots:].astype(BF)
    part = dot(d, jnp.concatenate([near_ref[:, :model], tok_ref[:, :model]], axis=0))
    count, high = mine_ref.shape[:2]
    own = model // (2 * count)
    pack = 128 // own
    part = jnp.concatenate([part, jnp.zeros((high * pack - part.shape[0], model), F32)], axis=0)
    for j in range(count):
        low = part[:, 2 * j * own : (2 * j + 1) * own]
        up = part[:, (2 * j + 1) * own : (2 * j + 2) * own]
        for ref, cols in (
            (mine_ref, jnp.where(core == 0, low, up)),
            (other_ref, jnp.where(core == 0, up, low)),
        ):
            ref[j] = jnp.concatenate(
                [cols[i * high : (i + 1) * high] for i in range(pack)], axis=1
            )


def collect_kernel(dims, stat_ref, y0_ref, y1_ref, mine_ref, other_ref):
    groups, width, _, slots = dims
    my_group, _, core = where_am_i(width)
    every = group_onehots(
        stat_ref[0:1, :], stat_ref[1:2, :], my_group, (core, groups - 1 - core), slots
    )
    total = dot_tn(every, jnp.concatenate([y0_ref[...], y1_ref[...]], axis=0)).astype(BF)
    half = mine_ref.shape[1]
    left, right = total[:, :half], total[:, half:]
    mine_ref[...] = jnp.where(core == 0, left, right)
    other_ref[...] = jnp.where(core == 0, right, left)


def final_kernel(mine_ref, other_ref, out_ref):
    out_ref[...] = (mine_ref[...].astype(F32) + other_ref[...].astype(F32)).astype(BF)


def body(tokens, cotangent, routes, router_group, router_expert, gate_proj, up_proj, down_proj):
    toks, model = tokens.shape
    top = routes.shape[1]
    groups = router_group.shape[1]
    experts = router_expert.shape[1]
    width = experts // groups
    cap = toks // width
    slots = width * cap // top
    ep = lax.axis_size("ep")
    tp = lax.axis_size("tp")
    half = model // tp
    hidden = gate_proj.shape[2]
    assert groups == 2 * tp and tp == 2
    dims = (groups, width, cap, slots)
    batch = 2 * width * cap
    flat = batch * model * hidden
    small = toks * toks * model

    def sds(shape, dtype=BF):
        return jax.ShapeDtypeStruct(shape, dtype)

    def over_groups(x, far):
        perm = []
        for i in range(ep):
            for c in range(tp):
                k = groups - 1 - c if far else c
                to = ((i // width) ^ k) * width + i % width
                perm.append((i * tp + c, to * tp + c))
        return lax.ppermute(x, ("ep", "tp"), perm)

    def over_members(blocks):
        moved = [blocks[0]]
        for k in range(1, width):
            moved.append(lax.ppermute(blocks[k], "ep", [(i, i ^ k) for i in range(ep)]))
        return moved

    def swap(x):
        return lax.ppermute(x, "tp", [(i, tp - 1 - i) for i in range(tp)])

    near, z_t, z_c, stat = call(
        functools.partial(prep_kernel, dims),
        [
            sds((slots, 2 * model + 128)),
            sds((slots, model + 128)),
            sds((slots, model)),
            sds((8, toks), F32),
        ],
        (tokens, cotangent, routes.T, router_group.T, router_expert.T),
        scratch=[
            pltpu.VMEM((toks, model), BF),
            pltpu.VMEM((toks, model), BF),
            pltpu.VMEM((top, toks), jnp.int32),
            pltpu.VMEM((groups, model), BF),
            pltpu.VMEM((experts, model), BF),
            pltpu.SemaphoreType.DMA((5,)),
        ],
        in_hbm=(0, 1, 2, 3, 4),
        limit=60 * 2**20,
        flops=4 * small,
    )
    z_t = over_groups(z_t, True)
    near = over_groups(near, False)
    z_c = over_groups(z_c, True)

    def spread(blocks, cols):
        return call(
            functools.partial(spread_kernel, dims),
            [sds((cap, cols))] * width,
            blocks,
            flops=4 * small,
        )

    m_a = over_members(spread((near,), 2 * model + 128))
    m_t = over_members(spread((z_t,), model + 128))
    m_c = over_members(spread((z_t, z_c), model))
    gate_mat, up_mat, down_mat = gate_proj[0], up_proj[0], down_proj[0]
    gates = (gate_mat, swap(gate_mat))
    ups = (up_mat, swap(up_mat))
    downs = (down_mat, swap(down_mat))
    x_full, *pre = call(
        functools.partial(forward_kernel, width),
        [sds((batch, model))] + [sds((batch, hidden), F32)] * 4,
        (*m_a, *m_t, *gates, *ups),
        flops=8 * flat,
    )
    mine, other, c_full, w_cols, *back = call(
        functools.partial(delta_kernel, width),
        [sds((batch, 3 * hidden))] * 2
        + [sds((batch, model)), sds((batch, 128), F32)]
        + [sds((2 * cap, model + 128))] * width,
        (*m_a, *m_c, *m_t, *gates, *ups, *downs, *pre),
        flops=12 * flat,
    )
    back = over_members(back)
    got = swap(other)
    x_other = swap(x_full)
    scaled = call(scale_kernel, sds((batch, model)), (c_full, w_cols), flops=small)
    scaled_other = swap(scaled)
    gate_grad, up_grad, in_sq = call(
        grad_kernel,
        [sds((model, hidden))] * 2 + [sds((2, model), F32)],
        (x_full, x_other, mine, got),
        scratch=[pltpu.VMEM((2 * batch, hidden), BF)] * 2,
        flops=8 * flat,
    )
    down_grad, dsq = call(
        down_kernel,
        [sds((hidden, model)), sds((1, hidden), F32)],
        (scaled, scaled_other, mine, got),
        scratch=[pltpu.VMEM((hidden, 128), F32), pltpu.VMEM((hidden, 2 * batch), BF)],
        flops=4 * flat,
    )
    own = model // (ep * tp)
    high = -(-(experts + 8) // (8 * (128 // own))) * 8
    routers = jnp.concatenate(
        [router_expert.T, router_group.T, jnp.zeros((8 - groups, model), BF)], axis=0
    )
    y_near, y_far, part, part_other = call(
        functools.partial(merge_kernel, dims, experts),
        [sds((slots, model))] * 2 + [sds((ep, high, 128), F32)] * 2,
        (routers, near, z_t, *back),
        flops=4 * small,
    )
    y_far = over_groups(y_far, True)
    y_near = over_groups(y_near, False)
    part = part + swap(part_other)
    part = lax.all_to_all(part, "ep", split_axis=0, concat_axis=0, tiled=True)
    by_expert, by_group, router_rows, gsq, usq = call(
        functools.partial(reduce_kernel, (experts, groups, own)),
        [sds((experts, own), F32), sds((groups, own), F32), sds((1, own), F32)]
        + [sds((1, model), F32)] * 2,
        (part, in_sq, swap(in_sq)),
        flops=small // 8,
    )
    left, right = call(
        functools.partial(collect_kernel, dims),
        [sds((toks, half))] * 2,
        (stat, y_near, y_far),
        flops=2 * small,
    )
    token_grad = call(final_kernel, sds((toks, half)), (left, swap(right)), flops=small)
    return (
        token_grad,
        gate_grad[None],
        up_grad[None],
        down_grad[None],
        gsq,
        usq,
        dsq,
        by_expert.T,
        by_group.T,
        router_rows.reshape(own),
    )


def solution(mesh):
    return jax.shard_map(
        body,
        mesh=mesh,
        in_specs=(
            P("ep", None),
            P("ep", None),
            P("ep", None),
            P(),
            P(),
            P("ep", None, "tp"),
            P("ep", None, "tp"),
            P("ep", "tp", None),
        ),
        out_specs=(
            P("ep", "tp"),
            P("ep", None, "tp"),
            P("ep", None, "tp"),
            P("ep", "tp", None),
            P("ep", None),
            P("ep", None),
            P("ep", "tp"),
            P(("ep", "tp"), None),
            P(("ep", "tp"), None),
            P(("ep", "tp")),
        ),
        check_vma=False,
    )
```

```python
import functools

import jax
import jax.numpy as jnp
from jax import lax
from jax.experimental import pallas as pl
from jax.experimental.pallas import tpu as pltpu
from jax.sharding import PartitionSpec as P


BF = jnp.bfloat16
F32 = jnp.float32


def dot(a, b):
    return jnp.dot(a, b, preferred_element_type=F32)


def dot_nt(a, b):
    return lax.dot_general(a, b, (((1,), (1,)), ((), ())), preferred_element_type=F32)


def dot_tn(a, b):
    return lax.dot_general(a, b, (((0,), (0,)), ((), ())), preferred_element_type=F32)


def iota(shape, axis):
    return lax.broadcasted_iota(jnp.int32, shape, axis)


def onehot(mask):
    return jnp.where(mask, 1.0, 0.0).astype(BF)


def where_am_i(width):
    ep, tp = lax.axis_index("ep"), lax.axis_index("tp")
    return ep // width, ep % width, tp


def call(kernel, out_shapes, args, scratch=(), flops=0, in_hbm=(), limit=24 * 2**20):
    vmem = pl.BlockSpec(memory_space=pltpu.VMEM)
    smem = pl.BlockSpec(memory_space=pltpu.SMEM)
    hbm = pl.BlockSpec(memory_space=pltpu.HBM)
    in_specs = [
        smem if a.ndim == 1 and a.dtype == jnp.int32 else hbm if i in in_hbm else vmem
        for i, a in enumerate(args)
    ]
    return pl.pallas_call(
        kernel,
        out_shape=out_shapes,
        in_specs=in_specs,
        out_specs=jax.tree.map(lambda _: vmem, out_shapes),
        scratch_shapes=list(scratch),
        cost_estimate=pl.CostEstimate(flops=flops, bytes_accessed=0, transcendentals=0),
        compiler_params=pltpu.CompilerParams(vmem_limit_bytes=limit),
    )(*args)


def group_onehots(rank_row, group_row, my_group, ks, slots):
    toks = rank_row.shape[1]
    hit = iota((slots, toks), 0).astype(F32) == rank_row
    outs = []
    for k in ks:
        other = jnp.bitwise_xor(my_group, k).astype(F32)
        outs.append(onehot(jnp.logical_and(hit, group_row == other)))
    return jnp.concatenate(outs, axis=0)


def slot_hits(shape, member, cap, per, s0, s1, slot_axis):
    slot = iota(shape, slot_axis)
    block = slot // per
    want = (jnp.bitwise_xor(member, block) * cap + slot % cap + 1).astype(F32)
    return s0 == want, s1 == want


def prep_kernel(dims, tok_hbm, cot_hbm, routes_hbm, rg_hbm, re_hbm, *rest):
    groups, width, cap, slots = dims
    near_ref, tok_out, cot_out, stat_ref, tok_ref, cot_ref, routes_ref, rg_ref, re_ref, sems = rest
    toks, model = tok_ref.shape
    experts = re_ref.shape[0]
    my_group, _, core = where_am_i(width)
    copies = [
        pltpu.make_async_copy(src, dst, sems.at[i])
        for i, (src, dst) in enumerate(
            (
                (routes_hbm, routes_ref),
                (re_hbm, re_ref),
                (rg_hbm, rg_ref),
                (tok_hbm, tok_ref),
                (cot_hbm, cot_ref),
            )
        )
    ]
    for copy in copies:
        copy.start()
    earlier = onehot(iota((toks, toks), 0) < iota((toks, toks), 1))
    for copy in copies[:4]:
        copy.wait()
    tokens = tok_ref[...]
    e_t = dot_nt(re_ref[...], tokens)
    g_t = dot_nt(rg_ref[...], tokens)
    g_t = jnp.concatenate([g_t, jnp.zeros((8 - groups, toks), F32)], axis=0)
    routes = routes_ref[...].astype(F32)
    r0, r1 = routes[0:1], routes[1:2]
    grow = iota((8, toks), 0)
    gexp = jnp.where(grow < groups, jnp.exp(g_t), 0.0)
    gprob = gexp / jnp.sum(gexp, axis=0, keepdims=True)
    low = (grow * width).astype(F32)
    gmask = jnp.logical_and(r0 >= low, r0 < low + width)
    picked = jnp.sum(jnp.where(gmask, gprob, 0.0), axis=0, keepdims=True)
    group_row = jnp.sum(jnp.where(gmask, grow.astype(F32), 0.0), axis=0, keepdims=True)
    erow = iota((experts, toks), 0).astype(F32)
    a0, a1 = erow == r0, erow == r1
    eexp = jnp.exp(e_t)
    x0 = jnp.sum(jnp.where(a0, eexp, 0.0), axis=0, keepdims=True)
    x1 = jnp.sum(jnp.where(a1, eexp, 0.0), axis=0, keepdims=True)
    p0, p1 = x0 / (x0 + x1), x1 / (x0 + x1)
    cum = dot(onehot(jnp.logical_or(a0, a1)), earlier)
    rank0 = jnp.sum(jnp.where(a0, cum, 0.0), axis=0, keepdims=True)
    rank1 = jnp.sum(jnp.where(a1, cum, 0.0), axis=0, keepdims=True)
    gcum = dot(onehot(gmask), earlier)
    rank_g = jnp.sum(jnp.where(gmask, gcum, 0.0), axis=0, keepdims=True)
    base = group_row * width
    s0 = (r0 - base) * cap + rank0 + 1.0
    s1 = (r1 - base) * cap + rank1 + 1.0
    mrow = iota((128, toks), 0)
    meta = jnp.where(mrow == 0, picked * p0, 0.0)
    meta = jnp.where(mrow == 1, picked * p1, meta)
    meta = jnp.where(mrow == 2, s0, meta)
    meta = jnp.where(mrow == 3, s1, meta)
    for i, v in enumerate([picked, p0, p1] + [gprob[j : j + 1] for j in range(groups)]):
        top = v.astype(BF).astype(F32)
        meta = jnp.where(mrow == 4 + 2 * i, top, meta)
        meta = jnp.where(mrow == 5 + 2 * i, v - top, meta)
    meta = meta.astype(BF)
    stat_ref[...] = jnp.where(iota((8, toks), 0) == 0, rank_g, group_row)
    every = group_onehots(rank_g, group_row, my_group, (core, groups - 1 - core), slots)
    metas = dot_nt(every, meta).astype(BF)
    moved = dot(every, tokens).astype(BF)
    near_ref[:, :model] = moved[:slots]
    tok_out[:, :model] = moved[slots:]
    near_ref[:, 2 * model :] = metas[:slots]
    tok_out[:, model:] = metas[slots:]
    copies[4].wait()
    moved = dot(every, cot_ref[...]).astype(BF)
    near_ref[:, model : 2 * model] = moved[:slots]
    cot_out[...] = moved[slots:]


def spread_kernel(dims, meta_ref, *refs):
    _, width, cap, slots = dims
    member = where_am_i(width)[1]
    data, outs = refs[: len(refs) - width], refs[len(refs) - width :]
    tail = meta_ref.shape[1] - 128
    meta = meta_ref[:, tail:]
    rows = jnp.transpose(jnp.concatenate([meta.astype(F32), jnp.zeros((128 - slots, 128), F32)], axis=0))
    rows = rows[:, :slots]
    shape = (width * cap, slots)
    hit0, hit1 = slot_hits(shape, member, cap, cap, rows[2:3], rows[3:4], 0)
    hit0, hit1 = onehot(hit0), onehot(hit1)
    values = data[0][...] if data else meta_ref[:, :tail]
    spread = dot(hit0 + hit1, values).astype(BF)
    for k in range(width):
        outs[k][:, : values.shape[1]] = spread[k * cap : (k + 1) * cap]
    if not data:
        weight = dot(hit0, meta)[:, 0:1] + dot(hit1, meta)[:, 1:2]
        wide = jnp.broadcast_to(weight, (width * cap, 128)).astype(BF)
        for k in range(width):
            outs[k][:, tail:] = wide[k * cap : (k + 1) * cap]


def forward_kernel(width, *refs):
    first, second = refs[:width], refs[width : 2 * width]
    weights, x_ref, outs = refs[2 * width : 2 * width + 4], refs[-7], refs[-6:]
    model = x_ref.shape[1]
    cap = first[0].shape[0]
    for k in range(width):
        x_ref[k * cap : (k + 1) * cap, :] = first[k][:, :model]
        x_ref[(width + k) * cap : (width + k + 1) * cap, :] = second[k][:, :model]
    x = x_ref[...]
    for n in range(2):
        gate_pre, up_pre = dot(x, weights[n][...]), dot(x, weights[2 + n][...])
        hid_ref, gate_ref, up_ref = outs[3 * n : 3 * n + 3]
        sig = 1.0 / (1.0 + jnp.exp(-gate_pre))
        silu = gate_pre * sig
        hid_ref[...] = (silu * up_pre).astype(BF)
        gate_ref[...] = up_pre * sig * (1.0 + gate_pre * (1.0 - sig))
        up_ref[...] = silu


def delta_kernel(width, *refs):
    first, second, tok = refs[:width], refs[width : 2 * width], refs[2 * width : 3 * width]
    gates, ups, downs = refs[3 * width : 3 * width + 2], refs[3 * width + 2 : 3 * width + 4], refs[3 * width + 4 : 3 * width + 6]
    pre, outs = refs[3 * width + 6 : 3 * width + 12], refs[3 * width + 12 :]
    mine_ref, other_ref, c_ref, w_ref = outs[:4]
    backs = outs[4 : 4 + width]
    model = c_ref.shape[1]
    cap = first[0].shape[0]
    for k in range(width):
        low, up = slice(k * cap, (k + 1) * cap), slice((width + k) * cap, (width + k + 1) * cap)
        c_ref[low, :] = first[k][:, model : 2 * model]
        c_ref[up, :] = second[k][...]
        w_ref[low, :] = first[k][:, 2 * model :].astype(F32)
        w_ref[up, :] = tok[k][:, model:].astype(F32)
    c = c_ref[...]
    scale = w_ref[:, 0:1]
    hidden = gates[0].shape[1]
    s = None
    for n, out in enumerate((mine_ref, other_ref)):
        pulled = dot_nt(c, downs[n][...])
        hid_ref, gate_ref, up_ref = pre[3 * n : 3 * n + 3]
        hid = hid_ref[...]
        dh = scale * pulled
        out[:, :hidden] = (dh * gate_ref[...]).astype(BF)
        out[:, hidden : 2 * hidden] = (dh * up_ref[...]).astype(BF)
        out[:, 2 * hidden :] = hid
        part = jnp.sum(pulled * hid.astype(F32), axis=1, keepdims=True)
        s = part if s is None else s + part
    wide = jnp.broadcast_to(s, (s.shape[0], 128)).astype(BF)
    for k in range(width):
        backs[k][:cap, model:] = wide[k * cap : (k + 1) * cap]
        backs[k][cap:, model:] = wide[(width + k) * cap : (width + k + 1) * cap]
    step = 1024

    @pl.loop(0, model // step)
    def _(i):
        at = pl.ds(pl.multiple_of(i * step, step), step)
        term = None
        for n, out in enumerate((mine_ref, other_ref)):
            piece = dot_nt(out[:, :hidden], gates[n][at, :])
            piece += dot_nt(out[:, hidden : 2 * hidden], ups[n][at, :])
            term = piece if term is None else term + piece
        term = term.astype(BF)
        for k in range(width):
            backs[k][:cap, at] = term[k * cap : (k + 1) * cap]
            backs[k][cap:, at] = term[(width + k) * cap : (width + k + 1) * cap]


def scale_kernel(c_ref, w_ref, out_ref):
    out_ref[...] = (w_ref[:, 0:1] * c_ref[...].astype(F32)).astype(BF)


def fold(x):
    total = x[:, :128]
    for i in range(1, x.shape[1] // 128):
        total = total + x[:, i * 128 : (i + 1) * 128]
    return total


def grad_kernel(x_ref, other_ref, mine_ref, got_ref, gg_ref, ug_ref, sq_ref, gd_ref, ud_ref):
    rows, hidden = x_ref.shape[0], gd_ref.shape[1]
    for n, ref in enumerate((mine_ref, got_ref)):
        gd_ref[n * rows : (n + 1) * rows, :] = ref[:, :hidden]
        ud_ref[n * rows : (n + 1) * rows, :] = ref[:, hidden : 2 * hidden]
    step = 512

    @pl.loop(0, x_ref.shape[1] // step)
    def _(i):
        at = pl.ds(pl.multiple_of(i * step, step), step)
        xt = jnp.concatenate(
            [jnp.transpose(x_ref[:, at]), jnp.transpose(other_ref[:, at])], axis=1
        )
        for n, (d_ref, out) in enumerate(((gd_ref, gg_ref), (ud_ref, ug_ref))):
            total = dot(xt, d_ref[...])
            out[at, :] = total.astype(BF)
            part = jnp.transpose(fold(total * total))
            sq_ref[n : n + 1, at] = jnp.sum(part, axis=0, keepdims=True)


def down_kernel(c_ref, other_ref, mine_ref, got_ref, out_ref, sq_ref, acc, hid_t):
    rows, hidden = c_ref.shape[0], hid_t.shape[0]
    acc[...] = jnp.zeros_like(acc)
    hid_t[:, :rows] = jnp.transpose(mine_ref[:, 2 * hidden :])
    hid_t[:, rows:] = jnp.transpose(got_ref[:, 2 * hidden :])
    step = 512

    @pl.loop(0, c_ref.shape[1] // step)
    def _(i):
        at = pl.ds(pl.multiple_of(i * step, step), step)
        total = dot(hid_t[...], jnp.concatenate([c_ref[:, at], other_ref[:, at]], axis=0))
        out_ref[:, at] = total.astype(BF)
        acc[...] += fold(total * total)

    sq_ref[...] = jnp.sum(jnp.transpose(acc[...]), axis=0, keepdims=True)


def reduce_kernel(dims, got_ref, sq_ref, sq_other_ref, e_ref, g_ref, rows_ref, gsq_ref, usq_ref):
    experts, groups, own = dims
    total = jnp.sum(got_ref[...], axis=0)
    pack = 128 // own
    total = jnp.concatenate([total[:, i * own : (i + 1) * own] for i in range(pack)], axis=0)
    by_expert, by_group = total[:experts], total[experts : experts + groups]
    e_ref[...] = by_expert
    g_ref[...] = by_group
    rows_ref[...] = jnp.sum(by_expert * by_expert, axis=0, keepdims=True) + jnp.sum(
        by_group * by_group, axis=0, keepdims=True
    )
    gsq_ref[...] = sq_ref[0:1] + sq_other_ref[0:1]
    usq_ref[...] = sq_ref[1:2] + sq_other_ref[1:2]


def merge_kernel(dims, experts, rt_ref, near_ref, tok_ref, *refs):
    groups, width, cap, slots = dims
    blocks, (y0_ref, y1_ref, mine_ref, other_ref) = refs[:width], refs[width:]
    my_group, member, core = where_am_i(width)
    model = y0_ref.shape[1]
    meta = jnp.concatenate([near_ref[:, 2 * model :], tok_ref[:, model:]], axis=0).astype(F32)
    toks = 2 * slots
    shape = (toks, width * 2 * cap)
    same = iota(shape, 1) // cap % 2 == iota(shape, 0) // slots
    hit0, hit1 = slot_hits(shape, member, cap, 2 * cap, meta[:, 2:3], meta[:, 3:4], 1)
    hit0, hit1 = onehot(jnp.logical_and(same, hit0)), onehot(jnp.logical_and(same, hit1))
    sent = jnp.concatenate([r[:, model:] for r in blocks], axis=0)
    lane = iota(meta.shape, 1)
    meta = jnp.where(lane == 126, dot(hit0, sent), meta)
    meta = jnp.where(lane == 127, dot(hit1, sent), meta)
    rows = jnp.transpose(meta)
    picked, p0, p1 = [rows[4 + 2 * i : 5 + 2 * i] + rows[5 + 2 * i : 6 + 2 * i] for i in range(3)]
    s0, s1 = rows[126:127], rows[127:128]
    dpicked = s0 * p0 + s1 * p1
    q0, q1 = picked * s0, picked * s1
    mean = p0 * q0 + p1 * q1
    c0, c1 = p0 * (q0 - mean), p1 * (q1 - mean)
    grow = iota((8, toks), 0)
    dgroup = jnp.zeros((8, toks), F32)
    for j in range(groups):
        at = 10 + 2 * j
        prob = rows[at : at + 1] + rows[at + 1 : at + 2]
        hot = jnp.where(my_group == j, 1.0, 0.0)
        dgroup = jnp.where(grow == j, dpicked * picked * (hot - prob), dgroup)
    erow = ((iota((experts, toks), 0) - my_group * width) * cap).astype(F32)
    dexpert = jnp.zeros((experts, toks), F32)
    for c, slot in ((c0, rows[2:3]), (c1, rows[3:4])):
        inside = jnp.logical_and(slot > erow, slot <= erow + cap)
        dexpert += jnp.where(inside, c, 0.0)
    d = jnp.concatenate([dexpert, dgroup], axis=0).astype(BF)
    total = dot(hit0 + hit1, jnp.concatenate([r[:, :model] for r in blocks], axis=0))
    total += dot_tn(d, rt_ref[...])
    y0_ref[...] = total[:slots].astype(BF)
    y1_ref[...] = total[slots:].astype(BF)
    part = dot(d, jnp.concatenate([near_ref[:, :model], tok_ref[:, :model]], axis=0))
    count, high = mine_ref.shape[:2]
    own = model // (2 * count)
    pack = 128 // own
    part = jnp.concatenate([part, jnp.zeros((high * pack - part.shape[0], model), F32)], axis=0)
    for j in range(count):
        low = part[:, 2 * j * own : (2 * j + 1) * own]
        up = part[:, (2 * j + 1) * own : (2 * j + 2) * own]
        for ref, cols in (
            (mine_ref, jnp.where(core == 0, low, up)),
            (other_ref, jnp.where(core == 0, up, low)),
        ):
            ref[j] = jnp.concatenate(
                [cols[i * high : (i + 1) * high] for i in range(pack)], axis=1
            )


def collect_kernel(dims, stat_ref, y0_ref, y1_ref, mine_ref, other_ref):
    groups, width, _, slots = dims
    my_group, _, core = where_am_i(width)
    every = group_onehots(
        stat_ref[0:1, :], stat_ref[1:2, :], my_group, (core, groups - 1 - core), slots
    )
    total = dot_tn(every, jnp.concatenate([y0_ref[...], y1_ref[...]], axis=0)).astype(BF)
    half = mine_ref.shape[1]
    left, right = total[:, :half], total[:, half:]
    mine_ref[...] = jnp.where(core == 0, left, right)
    other_ref[...] = jnp.where(core == 0, right, left)


def final_kernel(mine_ref, other_ref, out_ref):
    out_ref[...] = (mine_ref[...].astype(F32) + other_ref[...].astype(F32)).astype(BF)


def body(tokens, cotangent, routes, router_group, router_expert, gate_proj, up_proj, down_proj):
    toks, model = tokens.shape
    top = routes.shape[1]
    groups = router_group.shape[1]
    experts = router_expert.shape[1]
    width = experts // groups
    cap = toks // width
    slots = width * cap // top
    ep = lax.axis_size("ep")
    tp = lax.axis_size("tp")
    half = model // tp
    hidden = gate_proj.shape[2]
    assert groups == 2 * tp and tp == 2
    dims = (groups, width, cap, slots)
    batch = 2 * width * cap
    flat = batch * model * hidden
    small = toks * toks * model

    def sds(shape, dtype=BF):
        return jax.ShapeDtypeStruct(shape, dtype)

    def over_groups(x, far):
        perm = []
        for i in range(ep):
            for c in range(tp):
                k = groups - 1 - c if far else c
                to = ((i // width) ^ k) * width + i % width
                perm.append((i * tp + c, to * tp + c))
        return lax.ppermute(x, ("ep", "tp"), perm)

    def over_members(blocks):
        moved = [blocks[0]]
        for k in range(1, width):
            moved.append(lax.ppermute(blocks[k], "ep", [(i, i ^ k) for i in range(ep)]))
        return moved

    def swap(x):
        return lax.ppermute(x, "tp", [(i, tp - 1 - i) for i in range(tp)])

    near, z_t, z_c, stat = call(
        functools.partial(prep_kernel, dims),
        [
            sds((slots, 2 * model + 128)),
            sds((slots, model + 128)),
            sds((slots, model)),
            sds((8, toks), F32),
        ],
        (tokens, cotangent, routes.T, router_group.T, router_expert.T),
        scratch=[
            pltpu.VMEM((toks, model), BF),
            pltpu.VMEM((toks, model), BF),
            pltpu.VMEM((top, toks), jnp.int32),
            pltpu.VMEM((groups, model), BF),
            pltpu.VMEM((experts, model), BF),
            pltpu.SemaphoreType.DMA((5,)),
        ],
        in_hbm=(0, 1, 2, 3, 4),
        limit=60 * 2**20,
        flops=4 * small,
    )
    z_t = over_groups(z_t, True)
    near = over_groups(near, False)
    z_c = over_groups(z_c, True)

    def spread(blocks, cols):
        return call(
            functools.partial(spread_kernel, dims),
            [sds((cap, cols))] * width,
            blocks,
            flops=4 * small,
        )

    m_a = over_members(spread((near,), 2 * model + 128))
    m_t = over_members(spread((z_t,), model + 128))
    m_c = over_members(spread((z_t, z_c), model))
    gate_mat, up_mat, down_mat = gate_proj[0], up_proj[0], down_proj[0]
    gates = (gate_mat, swap(gate_mat))
    ups = (up_mat, swap(up_mat))
    downs = (down_mat, swap(down_mat))
    x_full, *pre = call(
        functools.partial(forward_kernel, width),
        [sds((batch, model))]
        + [sds((batch, hidden)), sds((batch, hidden), F32), sds((batch, hidden), F32)] * 2,
        (*m_a, *m_t, *gates, *ups),
        flops=8 * flat,
    )
    mine, other, c_full, w_cols, *back = call(
        functools.partial(delta_kernel, width),
        [sds((batch, 3 * hidden))] * 2
        + [sds((batch, model)), sds((batch, 128), F32)]
        + [sds((2 * cap, model + 128))] * width,
        (*m_a, *m_c, *m_t, *gates, *ups, *downs, *pre),
        flops=12 * flat,
    )
    back = over_members(back)
    got = swap(other)
    x_other = swap(x_full)
    scaled = call(scale_kernel, sds((batch, model)), (c_full, w_cols), flops=small)
    scaled_other = swap(scaled)
    gate_grad, up_grad, in_sq = call(
        grad_kernel,
        [sds((model, hidden))] * 2 + [sds((2, model), F32)],
        (x_full, x_other, mine, got),
        scratch=[pltpu.VMEM((2 * batch, hidden), BF)] * 2,
        flops=8 * flat,
    )
    down_grad, dsq = call(
        down_kernel,
        [sds((hidden, model)), sds((1, hidden), F32)],
        (scaled, scaled_other, mine, got),
        scratch=[pltpu.VMEM((hidden, 128), F32), pltpu.VMEM((hidden, 2 * batch), BF)],
        flops=4 * flat,
    )
    own = model // (ep * tp)
    high = -(-(experts + 8) // (8 * (128 // own))) * 8
    routers = jnp.concatenate(
        [router_expert.T, router_group.T, jnp.zeros((8 - groups, model), BF)], axis=0
    )
    y_near, y_far, part, part_other = call(
        functools.partial(merge_kernel, dims, experts),
        [sds((slots, model))] * 2 + [sds((ep, high, 128), F32)] * 2,
        (routers, near, z_t, *back),
        flops=4 * small,
    )
    y_far = over_groups(y_far, True)
    y_near = over_groups(y_near, False)
    part = part + swap(part_other)
    part = lax.all_to_all(part, "ep", split_axis=0, concat_axis=0, tiled=True)
    by_expert, by_group, router_rows, gsq, usq = call(
        functools.partial(reduce_kernel, (experts, groups, own)),
        [sds((experts, own), F32), sds((groups, own), F32), sds((1, own), F32)]
        + [sds((1, model), F32)] * 2,
        (part, in_sq, swap(in_sq)),
        flops=small // 8,
    )
    left, right = call(
        functools.partial(collect_kernel, dims),
        [sds((toks, half))] * 2,
        (stat, y_near, y_far),
        flops=2 * small,
    )
    token_grad = call(final_kernel, sds((toks, half)), (left, swap(right)), flops=small)
    return (
        token_grad,
        gate_grad[None],
        up_grad[None],
        down_grad[None],
        gsq,
        usq,
        dsq,
        by_expert.T,
        by_group.T,
        router_rows.reshape(own),
    )


def solution(mesh):
    return jax.shard_map(
        body,
        mesh=mesh,
        in_specs=(
            P("ep", None),
            P("ep", None),
            P("ep", None),
            P(),
            P(),
            P("ep", None, "tp"),
            P("ep", None, "tp"),
            P("ep", "tp", None),
        ),
        out_specs=(
            P("ep", "tp"),
            P("ep", None, "tp"),
            P("ep", None, "tp"),
            P("ep", "tp", None),
            P("ep", None),
            P("ep", None),
            P("ep", "tp"),
            P(("ep", "tp"), None),
            P(("ep", "tp"), None),
            P(("ep", "tp")),
        ),
        check_vma=False,
    )
```
